32 devices in a mesh: grp: 2 (over y), sp: 4 (over z), tp: 4 (over x, core).
Axes of the slice: x: 2, y: 2, z: 4, core: 2. Of those that a mesh axis runs over, the one named last changes fastest.
Arguments:
- inputs: bfloat16 [2048, 2048], P(('grp', 'sp')), parts along dimension 0, may hold values from -6 to 6
- norm_gain: float32 [2048], replicated, may hold values from 0.1 to 1.9
- da_query_weight: bfloat16 [2048, 1024], P('sp', 'tp'), may hold values from -0.125 to 0.125
- da_key_weight: bfloat16 [2048, 1024], P('sp', 'tp'), may hold values from -0.125 to 0.125
- da_value_weight: bfloat16 [2048, 1024], P('sp', 'tp'), may hold values from -0.125 to 0.125
- sw_query_weight: bfloat16 [2048, 1024], P('sp', 'tp'), may hold values from -0.125 to 0.125
- sw_key_weight: bfloat16 [2048, 512], P('sp', 'tp'), may hold values from -0.125 to 0.125
- sw_value_weight: bfloat16 [2048, 512], P('sp', 'tp'), may hold values from -0.125 to 0.125
- da_query_gain: float32 [64], replicated, may hold values from 0.6 to 30
- da_key_gain: float32 [64], replicated, may hold values from 0.6 to 30
- sw_query_gain: float32 [64], replicated, may hold values from 0.6 to 30
- sw_key_gain: float32 [64], replicated, may hold values from 0.6 to 30
- mix_lambda: float32 [8], P('tp'), may hold values from 0.3 to 0.8
- head_gain: float32 [128], replicated, may hold values from 0.1 to 1.9
- sink_logit: float32 [16], P('tp'), may hold values from 0 to 8
- da_out_weight: bfloat16 [1024, 2048], P('tp'), may hold values from -0.1875 to 0.1875
- sw_out_weight: bfloat16 [1024, 2048], P('tp'), may hold values from -0.1875 to 0.1875
Outputs:
- mixed: bfloat16 [2048, 2048], P(('grp', 'sp')), parts along dimension 0
The draws below stay inside these ranges and needn't reach their ends.
There are 2 independent parts, one for each index of `grp`. The reference program is written for one: setup_inputs(seed, part) draws one part's arguments, and reference() takes and returns one part's arrays. A program takes and returns all parts, laid end to end along the dimension named above; an argument that names none is the same for every part. Nothing has to cross between parts.
All inputs are finite; a program needn't handle non-finite values.
Results may differ from the reference program's by a relative error of at most 0.014.
The reference program's roundings to bfloat16 on the way count: a program that leaves them out, or rounds other values in their place, can miss the bound.
Values may be sent and summed in bfloat16 or wider, within the bound.
No kernel may reach another device: no remote copies, remote signals or barrier semaphores. Data moves between devices by JAX's collectives and lax.ppermute only.
A program may use at most 64 MiB of HBM per device.

```python
import math
import jax
import jax.numpy as jnp
from jax import lax

D = 2048
DA_HEADS = 8
SW_HEADS = 16
KV_HEADS = 8
HD = 64
WINDOW = 128
SEQ = 1024
N_TP = 4


def gain_draw(key, own):
    values = jax.random.uniform(jax.random.fold_in(key, own), (HD,), jnp.float32, 0.6, 2.4)
    return values


def draw_da_query_gain(key, part):
    return gain_draw(key, 11)


def draw_da_key_gain(key, part):
    return gain_draw(key, 12)


def draw_sw_query_gain(key, part):
    return gain_draw(key, 13)


def draw_sw_key_gain(key, part):
    return gain_draw(key, 14)


def level_of(key, extent, cuts, smallest, top_value):
    def one(dim, shards_of):
        steps = jax.random.uniform(jax.random.fold_in(jax.random.fold_in(key, 6), dim), (shards_of,), jnp.float32, smallest / len(cuts), top_value / len(cuts))
        return jnp.repeat(jnp.exp(steps), extent[dim] // shards_of).reshape((-1,) + (1,) * (len(extent) - dim - 1))

    loudness = one(*cuts[0])
    for cut in cuts[1:]:
        loudness = loudness * one(*cut)
    return loudness


def bell_draw(key, shape, width, reach, shards=(), held_as=jnp.bfloat16):
    entries = width * jax.random.normal(key, shape, jnp.float32)
    if shards:
        entries = entries * level_of(key, shape, shards, -0.22, 0.18)
    return jnp.clip(entries, -reach, reach).astype(held_as)


def setup_inputs(seed: int = 0, part: int = 0) -> dict:
    keys = jax.random.split(jax.random.key(seed), 18)
    own_keys = jax.random.split(jax.random.fold_in(keys[17], part), 18)
    inputs = bell_draw(own_keys[0], (SEQ, D), 1.0, 6.0, ((0, 4),))
    norm_gain = jnp.clip(1.0 + 0.18 * jax.random.normal(keys[1], (D,), jnp.float32), 0.1, 1.9)
    da_query_weight = bell_draw(keys[2], (D, DA_HEADS * 2 * HD), D ** -0.5, 0.125, ((0, 4), (1, 4)))
    da_key_weight = bell_draw(keys[3], (D, DA_HEADS * 2 * HD), D ** -0.5, 0.125, ((0, 4), (1, 4)))
    da_value_weight = bell_draw(keys[4], (D, DA_HEADS * 2 * HD), D ** -0.5, 0.125, ((0, 4), (1, 4)))
    sw_query_weight = bell_draw(keys[5], (D, SW_HEADS * HD), D ** -0.5, 0.125, ((0, 4), (1, 4)))
    sw_key_weight = bell_draw(keys[6], (D, KV_HEADS * HD), D ** -0.5, 0.125, ((0, 4), (1, 4)))
    sw_value_weight = bell_draw(keys[7], (D, KV_HEADS * HD), D ** -0.5, 0.125, ((0, 4), (1, 4)))
    da_query_gain = draw_da_query_gain(jax.random.fold_in(keys[17], 71), part)
    da_key_gain = draw_da_key_gain(jax.random.fold_in(keys[17], 71), part)
    sw_query_gain = draw_sw_query_gain(jax.random.fold_in(keys[17], 71), part)
    sw_key_gain = draw_sw_key_gain(jax.random.fold_in(keys[17], 71), part)
    mix_lambda = jnp.clip(0.3 + 0.5 * jax.random.uniform(keys[12], (DA_HEADS,), jnp.float32) ** level_of(keys[12], (DA_HEADS,), ((0, 4),), -0.2, 0.2), 0.3, 0.8)
    head_gain = jnp.clip(1.0 + 0.18 * jax.random.normal(keys[13], (2 * HD,), jnp.float32), 0.1, 1.9)
    sink_logit = jnp.clip(8.0 * jax.random.uniform(keys[14], (SW_HEADS,), jnp.float32) ** level_of(keys[14], (SW_HEADS,), ((0, 4),), -0.2, 0.2), 0.0, 8.0)
    da_out_weight = bell_draw(keys[15], (DA_HEADS * 2 * HD, D), (DA_HEADS * 2 * HD) ** -0.5, 0.1875, ((0, 4),))
    sw_out_weight = bell_draw(keys[16], (SW_HEADS * HD, D), (SW_HEADS * HD) ** -0.5, 0.1875, ((0, 4),))
    return {"inputs": inputs, "norm_gain": norm_gain, "da_query_weight": da_query_weight, "da_key_weight": da_key_weight, "da_value_weight": da_value_weight, "sw_query_weight": sw_query_weight, "sw_key_weight": sw_key_weight, "sw_value_weight": sw_value_weight, "da_query_gain": da_query_gain, "da_key_gain": da_key_gain, "sw_query_gain": sw_query_gain, "sw_key_gain": sw_key_gain, "mix_lambda": mix_lambda, "head_gain": head_gain, "sink_logit": sink_logit, "da_out_weight": da_out_weight, "sw_out_weight": sw_out_weight}


def rms_norm(values, gain):
    return values * lax.rsqrt(lax.optimization_barrier(jnp.mean(values * values, axis=-1, keepdims=True)) + 1e-06) * gain

def reference(inputs, norm_gain, da_query_weight, da_key_weight, da_value_weight, sw_query_weight, sw_key_weight, sw_value_weight, da_query_gain, da_key_gain, sw_query_gain, sw_key_gain, mix_lambda, head_gain, sink_logit, da_out_weight, sw_out_weight):
    length = inputs.shape[0]
    normed = rms_norm(inputs.astype(jnp.float32), norm_gain).astype(jnp.bfloat16)

    def project(matrix):
        return jnp.dot(normed, matrix, preferred_element_type=jnp.float32)
    da_query = rms_norm(project(da_query_weight).reshape(length, DA_HEADS, 2, HD), da_query_gain).astype(jnp.bfloat16)
    da_key = rms_norm(project(da_key_weight).reshape(length, DA_HEADS, 2, HD), da_key_gain).astype(jnp.bfloat16)
    da_value = project(da_value_weight).astype(jnp.bfloat16).reshape(length, DA_HEADS, 2 * HD)
    sw_query = rms_norm(project(sw_query_weight).reshape(length, SW_HEADS, HD), sw_query_gain).astype(jnp.bfloat16)
    sw_key = rms_norm(project(sw_key_weight).reshape(length, KV_HEADS, HD), sw_key_gain).astype(jnp.bfloat16)
    sw_value = project(sw_value_weight).astype(jnp.bfloat16).reshape(length, KV_HEADS, HD)
    scale = HD ** (-0.5)
    block = math.gcd(length, 512)
    positions = jnp.arange(length, dtype=jnp.int32)
    keys_wide = da_key.astype(jnp.float32)
    values_wide = da_value.astype(jnp.float32)

    def da_block(first):
        rows = lax.dynamic_slice_in_dim(da_query, first, block, 0).astype(jnp.float32)
        scores = jnp.einsum('qhmd,khmd->hmqk', rows, keys_wide) * scale
        here = first + jnp.arange(block, dtype=jnp.int32)
        scores = jnp.where(positions[None, :] <= here[:, None], scores, -jnp.inf)
        top = lax.optimization_barrier(jnp.max(scores, axis=-1, keepdims=True))
        weights = jnp.exp(scores - top)
        total = lax.optimization_barrier(jnp.sum(weights, axis=-1))
        rounded = lax.optimization_barrier(weights.astype(jnp.bfloat16)).astype(jnp.float32)
        summed = jnp.einsum('hmqk,khe->hmqe', rounded, values_wide)
        maps = summed / total[..., None]
        blend = maps[:, 0] - mix_lambda[:, None, None] * maps[:, 1]
        return jnp.transpose(blend, (1, 0, 2))
    starts = jnp.arange(length // block, dtype=jnp.int32) * block
    blend_all = lax.map(da_block, starts).reshape(length, DA_HEADS, 2 * HD)
    da_rows = rms_norm(blend_all, head_gain).astype(jnp.bfloat16).reshape(length, DA_HEADS * 2 * HD)
    groups = SW_HEADS // KV_HEADS
    count = length // WINDOW

    def band(array):
        tiles = array.astype(jnp.float32).reshape(count, WINDOW, KV_HEADS, HD)
        earlier = jnp.concatenate([jnp.zeros_like(tiles[:1]), tiles[:-1]], axis=0)
        return jnp.concatenate([earlier, tiles], axis=1)
    key_band = band(sw_key)
    value_band = band(sw_value)
    query_tiles = sw_query.astype(jnp.float32).reshape(count, WINDOW, KV_HEADS, groups, HD)
    scores = jnp.einsum('nqhgd,nkhd->nhgqk', query_tiles, key_band) * scale
    lag = WINDOW + jnp.arange(WINDOW)[:, None] - jnp.arange(2 * WINDOW)[None, :]
    key_places = jnp.arange(count)[:, None] * WINDOW - WINDOW + jnp.arange(2 * WINDOW)[None, :]
    valid = ((lag >= 0) & (lag < WINDOW))[None] & (key_places >= 0)[:, None, :]
    scores = jnp.where(valid[:, None, None], scores, -jnp.inf)
    sink = sink_logit.reshape(KV_HEADS, groups)[None, :, :, None]
    top = jnp.maximum(lax.optimization_barrier(jnp.max(scores, axis=-1)), sink)
    weights = jnp.exp(scores - top[..., None])
    total = lax.optimization_barrier(jnp.sum(weights, axis=-1)) + jnp.exp(sink - top)
    rounded = lax.optimization_barrier(weights.astype(jnp.bfloat16)).astype(jnp.float32)
    summed = jnp.einsum('nhgqk,nkhd->nqhgd', rounded, value_band)
    sw_rows = (summed / jnp.transpose(total, (0, 3, 1, 2))[..., None]).astype(jnp.bfloat16).reshape(length, SW_HEADS * HD)
    da_cols = DA_HEADS * 2 * HD // N_TP
    sw_cols = SW_HEADS * HD // N_TP
    mixed = jnp.zeros((length, D), jnp.float32)
    for member in range(N_TP):
        partial_value = jnp.dot(da_rows[:, member * da_cols:(member + 1) * da_cols], da_out_weight[member * da_cols:(member + 1) * da_cols], preferred_element_type=jnp.float32)
        partial_value = partial_value + jnp.dot(sw_rows[:, member * sw_cols:(member + 1) * sw_cols], sw_out_weight[member * sw_cols:(member + 1) * sw_cols], preferred_element_type=jnp.float32)
        mixed = mixed + lax.optimization_barrier(partial_value.astype(jnp.bfloat16)).astype(jnp.float32)
    return mixed.astype(jnp.bfloat16)
```

```python
import jax
import jax.numpy as jnp
from jax import lax
from jax.sharding import PartitionSpec as P

HD = 64
WINDOW = 128


def rotated(value, axis, steps):
    count = lax.axis_size(axis)
    return lax.ppermute(value, axis, [(i, (i + steps) % count) for i in range(count)])


def shifted(value, axis, steps):
    count = lax.axis_size(axis)
    first, last = (max(0, -steps), min(count, count - steps))
    return lax.ppermute(value, axis, [(source, source + steps) for source in range(first, last)])


def crossed(value, axis, mask):
    count = lax.axis_size(axis)
    return lax.ppermute(value, axis, [(i, i ^ mask) for i in range(count)])


def over_tp(value):
    count = lax.axis_size("tp")
    far = {0: value}
    for mask in range(2, count, 2):
        far[mask] = crossed(value, "tp", mask)
    result = []
    for mask in range(0, count, 2):
        result.append(far[mask])
        result.append(crossed(far[mask], "tp", 1))
    return result


def over_tp_direct(value):
    count = lax.axis_size("tp")
    return [value] + [crossed(value, "tp", mask) for mask in range(1, count)]


def rms_norm(values, gain):
    return values * lax.rsqrt(jnp.mean(values * values, axis=-1, keepdims=True) + 1e-06) * gain


def gathered_pieces(own):
    count, parts = lax.axis_size("sp"), lax.axis_size("grp")
    size = own.shape[0] // parts
    mine = lax.dynamic_slice_in_dim(own, lax.axis_index("grp") * size, size, 0)
    pieces = []
    for back in range(1, count):
        piece = rotated(mine, "sp", back)
        pieces.append((back, 0, piece))
        for other in range(1, parts):
            pieces.append((back, other, rotated(piece, "grp", other)))
    return pieces


def project(normed, own, pieces):
    count, parts = lax.axis_size("sp"), lax.axis_size("grp")
    place, part = lax.axis_index("sp"), lax.axis_index("grp")
    depth = own.shape[0]
    size = depth // parts
    total = jnp.dot(
        lax.dynamic_slice_in_dim(normed, place * depth, depth, 1),
        own,
        preferred_element_type=jnp.float32,
    )
    for back, other, piece in pieces:
        first = lax.rem(place - back + count, count) * depth
        first = first + lax.rem(part - other + parts, parts) * size
        columns = lax.dynamic_slice_in_dim(normed, first, size, 1)
        total = total + jnp.dot(columns, piece, preferred_element_type=jnp.float32)
    return total


def diff_attention(queries, places, keys, values, key_places, mix_lambda, head_gain):
    rows, heads = queries.shape[:2]
    scores = jnp.einsum(
        "qhmd,khmd->hmqk", queries, keys, preferred_element_type=jnp.float32
    ) * HD ** (-0.5)
    valid = (key_places[None, :] <= places[:, None]) & (key_places >= 0)[None, :]
    scores = jnp.where(valid, scores, -jnp.inf)
    top = jnp.max(scores, axis=-1)
    weights = jnp.exp(scores - top[..., None])
    total = jnp.sum(weights, axis=-1)
    summed = jnp.einsum(
        "hmqk,khe->hmqe", weights.astype(jnp.bfloat16), values, preferred_element_type=jnp.float32
    )
    maps = summed / total[..., None]
    blend = maps[:, 0] - mix_lambda[:, None, None] * maps[:, 1]
    blend = jnp.transpose(blend, (1, 0, 2))
    return rms_norm(blend, head_gain).astype(jnp.bfloat16).reshape(rows, heads * 2 * HD)


def window_attention(sw_query, sw_key, sw_value, earlier_key, earlier_value, sink_logit, first):
    rows = sw_query.shape[0]
    sw_heads = sw_query.shape[1]
    kv_heads = sw_key.shape[1]
    groups = sw_heads // kv_heads
    count = rows // WINDOW

    def band(own, earlier_tile):
        tiles = own.reshape(count, WINDOW, kv_heads, HD)
        earlier = jnp.concatenate([earlier_tile[None], tiles[:-1]], axis=0)
        return jnp.concatenate([earlier, tiles], axis=1)

    key_band = band(sw_key, earlier_key)
    value_band = band(sw_value, earlier_value)
    query_tiles = sw_query.reshape(count, WINDOW, kv_heads, groups, HD)
    scores = jnp.einsum(
        "nqhgd,nkhd->nhgqk", query_tiles, key_band, preferred_element_type=jnp.float32
    ) * HD ** (-0.5)
    lag = WINDOW + jnp.arange(WINDOW)[:, None] - jnp.arange(2 * WINDOW)[None, :]
    key_places = (
        first + jnp.arange(count)[:, None] * WINDOW - WINDOW + jnp.arange(2 * WINDOW)[None, :]
    )
    valid = ((lag >= 0) & (lag < WINDOW))[None] & (key_places >= 0)[:, None, :]
    scores = jnp.where(valid[:, None, None], scores, -jnp.inf)
    sink = sink_logit.reshape(kv_heads, groups)[None, :, :, None]
    top = jnp.maximum(jnp.max(scores, axis=-1), sink)
    weights = jnp.exp(scores - top[..., None])
    total = jnp.sum(weights, axis=-1) + jnp.exp(sink - top)
    summed = jnp.einsum(
        "nhgqk,nkhd->nqhgd",
        weights.astype(jnp.bfloat16),
        value_band,
        preferred_element_type=jnp.float32,
    )
    return (
        (summed / jnp.transpose(total, (0, 3, 1, 2))[..., None])
        .astype(jnp.bfloat16)
        .reshape(rows, sw_heads * HD)
    )


def on_device(
    inputs,
    norm_gain,
    da_query_weight,
    da_key_weight,
    da_value_weight,
    sw_query_weight,
    sw_key_weight,
    sw_value_weight,
    da_query_gain,
    da_key_gain,
    sw_query_gain,
    sw_key_gain,
    mix_lambda,
    head_gain,
    sink_logit,
    da_out_weight,
    sw_out_weight,
):
    rows = inputs.shape[0]
    count = lax.axis_size("sp")
    place = lax.axis_index("sp")
    first = place * rows
    places = first + jnp.arange(rows, dtype=jnp.int32)
    da_heads = da_query_weight.shape[1] // (2 * HD)
    sw_heads = sw_query_weight.shape[1] // HD
    kv_heads = sw_key_weight.shape[1] // HD

    own_kv = jnp.concatenate([da_key_weight, da_value_weight], axis=1)
    own_rest = jnp.concatenate(
        [da_query_weight, sw_query_weight, sw_key_weight, sw_value_weight], axis=1
    )
    kv_pieces = gathered_pieces(own_kv)
    rest_pieces = gathered_pieces(own_rest)
    da_out_weights = over_tp(da_out_weight)
    sw_out_weights = over_tp(sw_out_weight)

    normed = rms_norm(inputs.astype(jnp.float32), norm_gain).astype(jnp.bfloat16)

    kv = project(normed, own_kv, kv_pieces)
    width = da_key_weight.shape[1]
    da_key = rms_norm(kv[:, :width].reshape(rows, da_heads, 2, HD), da_key_gain)
    da_kv = jnp.concatenate(
        [da_key.astype(jnp.bfloat16).reshape(rows, width), kv[:, width:].astype(jnp.bfloat16)],
        axis=1,
    )
    all_kv = jnp.concatenate([da_kv] + [shifted(da_kv, "sp", back) for back in range(1, count)])
    key_places = jnp.concatenate([places - back * rows for back in range(count)])
    keys = all_kv[:, :width].reshape(-1, da_heads, 2, HD)
    values = all_kv[:, width:].reshape(-1, da_heads, 2 * HD)

    rest = project(normed, own_rest, rest_pieces)
    cuts = [da_query_weight.shape[1], sw_query_weight.shape[1], sw_key_weight.shape[1]]
    cuts = [sum(cuts[: i + 1]) for i in range(3)]
    da_query = rms_norm(rest[:, : cuts[0]].reshape(rows, da_heads, 2, HD), da_query_gain).astype(
        jnp.bfloat16
    )
    sw_query = rms_norm(
        rest[:, cuts[0] : cuts[1]].reshape(rows, sw_heads, HD), sw_query_gain
    ).astype(jnp.bfloat16)
    sw_key = rms_norm(rest[:, cuts[1] : cuts[2]].reshape(rows, kv_heads, HD), sw_key_gain).astype(
        jnp.bfloat16
    )
    sw_value = rest[:, cuts[2] :].astype(jnp.bfloat16).reshape(rows, kv_heads, HD)
    edge = jnp.stack([sw_key[rows - WINDOW :], sw_value[rows - WINDOW :]])
    earlier = shifted(edge, "sp", 1)
    sw_rows = window_attention(
        sw_query, sw_key, sw_value, earlier[0], earlier[1], sink_logit, first
    )
    all_sw_rows = over_tp_direct(sw_rows)
    da_rows = diff_attention(da_query, places, keys, values, key_places, mix_lambda, head_gain)
    all_da_rows = over_tp_direct(da_rows)
    mixed = jnp.zeros(inputs.shape, jnp.float32)
    for da, sw, da_out, sw_out in zip(all_da_rows, all_sw_rows, da_out_weights, sw_out_weights):
        partial_value = jnp.dot(da, da_out, preferred_element_type=jnp.float32) + jnp.dot(
            sw, sw_out, preferred_element_type=jnp.float32
        )
        mixed = mixed + partial_value.astype(jnp.bfloat16).astype(jnp.float32)
    return mixed.astype(jnp.bfloat16)


def solution(mesh):
    return jax.shard_map(
        on_device,
        mesh=mesh,
        in_specs=(
            P(("grp", "sp"), None),
            P(),
            P("sp", "tp"),
            P("sp", "tp"),
            P("sp", "tp"),
            P("sp", "tp"),
            P("sp", "tp"),
            P("sp", "tp"),
            P(),
            P(),
            P(),
            P(),
            P("tp"),
            P(),
            P("tp"),
            P("tp", None),
            P("tp", None),
        ),
        out_specs=P(("grp", "sp"), None),
        check_vma=False,
    )
```
